32 devices in a mesh: sp: 8 (over z, y), tp: 4 (over x, core).
Axes of the slice: x: 2, y: 2, z: 4, core: 2. Of those that a mesh axis runs over, the one named last changes fastest.
Arguments:
- resid: bfloat16 [6144, 2048], P(('sp', 'tp')), may hold values from -6 to 6
- query_small: bfloat16 [6144, 768], P('sp', 'tp'), may hold values from -480 to 480
- query_large: bfloat16 [6144, 1280], P('sp', 'tp'), may hold values from -480 to 480
- kv_latent: bfloat16 [6144, 256], P('sp'), may hold values from -6 to 6
- rope_key: bfloat16 [6144, 32], P('sp'), may hold values from -6 to 6
- kv_gain: bfloat16 [256], replicated, may hold values from 0.099609375 to 1.8984375
- up_key_small: bfloat16 [256, 512], P(None, 'tp'), may hold values from -0.375 to 0.375
- up_value_small: bfloat16 [256, 512], P(None, 'tp'), may hold values from -0.375 to 0.375
- up_key_large: bfloat16 [256, 1024], P(None, 'tp'), may hold values from -0.375 to 0.375
- up_value_large: bfloat16 [256, 1024], P(None, 'tp'), may hold values from -0.375 to 0.375
- out_weight: bfloat16 [1536, 2048], replicated, may hold values from -0.359375 to 0.359375
- mix_gain: bfloat16 [2048], replicated, may hold values from 0.099609375 to 1.8984375
- gate_weight: bfloat16 [2048, 5632], P('sp', 'tp'), may hold values from -0.125 to 0.125
- up_weight: bfloat16 [2048, 5632], P('sp', 'tp'), may hold values from -0.125 to 0.125
- down_weight: bfloat16 [2048, 5632], P('sp', 'tp'), may hold values from -0.078125 to 0.078125
Outputs:
- layer_output: bfloat16 [6144, 2048], P(('sp', 'tp'))
The draws below stay inside these ranges and needn't reach their ends.
All inputs are finite; a program needn't handle non-finite values.
Results may differ from the reference program's by a relative error of at most 0.014.
The reference program's roundings to bfloat16 on the way count: a program that leaves them out, or rounds other values in their place, can miss the bound.
Values may be sent and summed in bfloat16 or wider, within the bound.
No kernel may reach another device: no remote copies, remote signals or barrier semaphores. Data moves between devices by JAX's collectives and lax.ppermute only.
A program may use at most 128 MiB of HBM per device.

```python
import math
import jax
import jax.numpy as jnp
from jax import lax

D = 2048
HEADS_SMALL = 8
HEADS_LARGE = 8
NOPE_SMALL = 64
NOPE_LARGE = 128
VALUE_SMALL = 64
VALUE_LARGE = 128
ROTARY = 32
LATENT = 256
FF = 5632
TOK_DEV = 768
SEQ = 6144
N_TP = 4


def drawn_query(key, columns):
    base = 2.0 * jax.random.truncated_normal(key, -6.0, 6.0, (SEQ, columns), jnp.float32)
    return base


def draw_query_small(key, part):
    return drawn_query(jax.random.fold_in(key, 11), HEADS_SMALL * (NOPE_SMALL + ROTARY)).astype(jnp.bfloat16)


def draw_query_large(key, part):
    return drawn_query(jax.random.fold_in(key, 13), HEADS_LARGE * (NOPE_LARGE + ROTARY)).astype(jnp.bfloat16)


def steps_of(key, shape, split, low, high):
    loudness = 1.0
    for dim, shards_of in split:
        steps = jax.random.uniform(jax.random.fold_in(jax.random.fold_in(key, 6), dim), (shards_of,), jnp.float32, low / len(split), high / len(split))
        loudness = loudness * jnp.repeat(jnp.exp(steps), shape[dim] // shards_of).reshape((-1,) + (1,) * (len(shape) - 1 - dim))
    return loudness


def normal_values(own_key, extent, scale, bound, shards=(), held_as=jnp.bfloat16):
    factor_of = steps_of(own_key, extent, shards, -0.22, 0.18) if shards else 1.0
    drawn = jax.random.normal(own_key, extent, jnp.float32) * scale * factor_of
    return jnp.minimum(jnp.maximum(drawn, -bound), bound).astype(held_as)


def setup_inputs(seed: int = 0) -> dict:
    arg_keys = jax.random.split(jax.random.key(seed), 16)
    return {
        "resid": normal_values(arg_keys[0], (SEQ, D), 1.0, 6.0, ((0, 32),)),
        "query_small": draw_query_small(jax.random.fold_in(arg_keys[15], 71), 0),
        "query_large": draw_query_large(jax.random.fold_in(arg_keys[15], 71), 0),
        "kv_latent": normal_values(arg_keys[3], (SEQ, LATENT), 1.0, 6.0, ((0, 8),)),
        "rope_key": normal_values(arg_keys[4], (SEQ, ROTARY), 1.0, 6.0, ((0, 8),)),
        "kv_gain": jnp.clip(1.0 + 0.18 * jax.random.normal(arg_keys[5], (LATENT,), jnp.float32), 0.099609375, 1.8984375).astype(jnp.bfloat16),
        "up_key_small": normal_values(arg_keys[6], (LATENT, HEADS_SMALL * NOPE_SMALL), LATENT ** -0.5, 0.375, ((1, 4),)),
        "up_value_small": normal_values(arg_keys[7], (LATENT, HEADS_SMALL * VALUE_SMALL), LATENT ** -0.5, 0.375, ((1, 4),)),
        "up_key_large": normal_values(arg_keys[8], (LATENT, HEADS_LARGE * NOPE_LARGE), LATENT ** -0.5, 0.375, ((1, 4),)),
        "up_value_large": normal_values(arg_keys[9], (LATENT, HEADS_LARGE * VALUE_LARGE), LATENT ** -0.5, 0.375, ((1, 4),)),
        "out_weight": normal_values(arg_keys[10], (HEADS_SMALL * VALUE_SMALL + HEADS_LARGE * VALUE_LARGE, D), 0.06, 0.359375),
        "mix_gain": jnp.clip(1.0 + 0.18 * jax.random.normal(arg_keys[11], (D,), jnp.float32), 0.099609375, 1.8984375).astype(jnp.bfloat16),
        "gate_weight": normal_values(arg_keys[12], (D, FF), D ** -0.5, 0.125, ((0, 8), (1, 4))),
        "up_weight": normal_values(arg_keys[13], (D, FF), D ** -0.5, 0.125, ((0, 8), (1, 4))),
        "down_weight": normal_values(arg_keys[14], (D, FF), FF ** -0.5, 0.078125, ((0, 8), (1, 4))),
    }


THETA = 10000.0
EPSILON = 1e-06
FLOOR = -1e+30

def angles(positions, width):
    inverse = THETA ** (-jnp.arange(0, width, 2).astype(jnp.float32) / width)
    phase = positions.astype(jnp.float32)[:, None] * inverse[None, :]
    return (jnp.cos(phase), jnp.sin(phase))

def rotate(values, angle_cos, angle_sin):
    half = values.shape[-1] // 2
    first = values[..., :half].astype(jnp.float32)
    second = values[..., half:].astype(jnp.float32)
    turned = jnp.concatenate([first * angle_cos - second * angle_sin, second * angle_cos + first * angle_sin], axis=-1)
    return turned.astype(jnp.bfloat16)

def norm_rows(values, gain):
    wide = values.astype(jnp.float32)
    scaled = wide * lax.rsqrt(lax.optimization_barrier(jnp.mean(wide * wide, axis=-1, keepdims=True)) + EPSILON)
    return (scaled * gain.astype(jnp.float32)).astype(jnp.bfloat16)

def attend(query, key_nope, shared_key, values, nope):
    length = query.shape[0]
    heads = query.shape[1]
    scale = 1.0 / math.sqrt(nope + shared_key.shape[1])
    count = length // TOK_DEV
    key_wide = key_nope.astype(jnp.float32)
    shared_wide = shared_key.astype(jnp.float32)
    value_wide = values.astype(jnp.float32)

    def one_block(index):
        start = index * TOK_DEV
        block = lax.dynamic_slice_in_dim(query, start, TOK_DEV, 0).astype(jnp.float32)
        scores = jnp.einsum('qhd,khd->hqk', block[..., :nope], key_wide)
        scores = scores + jnp.einsum('qhd,kd->hqk', block[..., nope:], shared_wide)
        scores = scores * scale
        query_pos = start + jnp.arange(TOK_DEV).astype(jnp.int32)
        key_pos = jnp.arange(length).astype(jnp.int32)
        allowed = key_pos[None, :] <= query_pos[:, None]
        scores = jnp.where(allowed[None], scores, FLOOR)
        maximum = lax.optimization_barrier(jnp.max(scores, axis=-1, keepdims=True))
        weights = jnp.where(allowed[None], jnp.exp(scores - maximum), 0.0)
        total = lax.optimization_barrier(jnp.sum(weights, axis=-1))
        rounded = lax.optimization_barrier(weights.astype(jnp.bfloat16)).astype(jnp.float32)
        summed = jnp.einsum('hqk,khd->qhd', rounded, value_wide)
        return (summed / jnp.transpose(total)[:, :, None]).astype(jnp.bfloat16)
    out = lax.map(one_block, jnp.arange(count).astype(jnp.int32))
    return out.reshape(length, -1)

def reference(resid, query_small, query_large, kv_latent, rope_key, kv_gain, up_key_small, up_value_small, up_key_large, up_value_large, out_weight, mix_gain, gate_weight, up_weight, down_weight):
    length = kv_latent.shape[0]
    positions = jnp.arange(length).astype(jnp.int32)
    angle_cos, angle_sin = angles(positions, ROTARY)
    latent_normed = norm_rows(kv_latent, kv_gain)
    rotated_key = rotate(rope_key, angle_cos, angle_sin)

    def group(query, up_key, up_value, heads, nope, width):
        shaped = query.reshape(length, heads, nope + ROTARY)
        turned = rotate(shaped[..., nope:], angle_cos[:, None, :], angle_sin[:, None, :])
        full_query = jnp.concatenate([shaped[..., :nope], turned], axis=-1)
        keys = jnp.dot(latent_normed, up_key, preferred_element_type=jnp.float32).astype(jnp.bfloat16)
        values = jnp.dot(latent_normed, up_value, preferred_element_type=jnp.float32).astype(jnp.bfloat16)
        return attend(full_query, keys.reshape(length, heads, nope), rotated_key, values.reshape(length, heads, width), nope)
    attn_small = group(query_small, up_key_small, up_value_small, HEADS_SMALL, NOPE_SMALL, VALUE_SMALL)
    attn_large = group(query_large, up_key_large, up_value_large, HEADS_LARGE, NOPE_LARGE, VALUE_LARGE)
    border = HEADS_SMALL * VALUE_SMALL
    mixed = jnp.dot(attn_small, out_weight[:border], preferred_element_type=jnp.float32)
    mixed = mixed + jnp.dot(attn_large, out_weight[border:], preferred_element_type=jnp.float32)
    middle = (resid.astype(jnp.float32) + mixed).astype(jnp.bfloat16)
    middle_wide = lax.optimization_barrier(middle).astype(jnp.float32)
    mixer_in = norm_rows(middle, mix_gain)
    gate = jnp.dot(mixer_in, gate_weight, preferred_element_type=jnp.float32)
    upward = jnp.dot(mixer_in, up_weight, preferred_element_type=jnp.float32)
    hidden = (jax.nn.silu(gate) * upward).astype(jnp.bfloat16)
    width = FF // N_TP
    total = middle_wide
    for index in range(N_TP):
        part = jnp.dot(hidden[:, index * width:(index + 1) * width], jnp.transpose(down_weight[:, index * width:(index + 1) * width]), preferred_element_type=jnp.float32).astype(jnp.bfloat16)
        total = total + lax.optimization_barrier(part).astype(jnp.float32)
    return total.astype(jnp.bfloat16)
```

```python
import math

import jax
import jax.numpy as jnp
from jax import lax
from jax.experimental import pallas as pl
from jax.experimental.pallas import tpu as pltpu
from jax.sharding import PartitionSpec as P

HEADS_SMALL = 8
NOPE_SMALL = 64
NOPE_LARGE = 128
VALUE_SMALL = 64
VALUE_LARGE = 128
ROTARY = 32


THETA = 10000.0
EPSILON = 1e-06
FLOOR = -1e30


def angles(positions, width):
    inverse = THETA ** (-jnp.arange(0, width, 2).astype(jnp.float32) / width)
    phase = positions.astype(jnp.float32)[:, None] * inverse[None, :]
    return (jnp.cos(phase), jnp.sin(phase))


def rotate(values, angle_cos, angle_sin):
    half = values.shape[-1] // 2
    first = values[..., :half].astype(jnp.float32)
    second = values[..., half:].astype(jnp.float32)
    turned = jnp.concatenate(
        [first * angle_cos - second * angle_sin, second * angle_cos + first * angle_sin], axis=-1
    )
    return turned.astype(jnp.bfloat16)


def norm_rows(values, gain):
    wide = values.astype(jnp.float32)
    scaled = wide * lax.rsqrt(jnp.mean(wide * wide, axis=-1, keepdims=True) + EPSILON)
    return (scaled * gain.astype(jnp.float32)).astype(jnp.bfloat16)

LANES = 128
TILE = 256
LOG2E = math.log2(math.e)


def grid_of(count):
    inner = 1
    while inner * inner * 4 <= count and count % (inner * 2) == 0:
        inner *= 2
    return count // inner, inner


def shift(values, axis, outer, inner, step_outer, step_inner):
    pairs = [
        (a * inner + b, (a + step_outer) % outer * inner + (b + step_inner) % inner)
        for a in range(outer)
        for b in range(inner)
    ]
    return lax.ppermute(values, axis, pairs)


def gather_pieces(values, axis, outer, inner):
    pieces = [(0, 0, values)]
    for a in range(1, outer):
        pieces.append((a, 0, shift(values, axis, outer, inner, a, 0)))
    for a, _, held in list(pieces):
        for b in range(1, inner):
            pieces.append((a, b, shift(held, axis, outer, inner, 0, b)))
    return pieces


def gather_rows(values, axis, outer, inner):
    index = lax.axis_index(axis)
    here_outer, here_inner = index // inner, index % inner
    rows = values.shape[0]
    whole = jnp.zeros((outer * inner * rows,) + values.shape[1:], values.dtype)
    for a, b, piece in gather_pieces(values, axis, outer, inner):
        source = (here_outer - a) % outer * inner + (here_inner - b) % inner
        whole = lax.dynamic_update_slice_in_dim(whole, piece, source * rows, 0)
    return whole


def padded(values, before, width):
    spare = width - before - values.shape[-1]
    return jnp.pad(values, [(0, 0)] * (values.ndim - 1) + [(before, spare)])


def attend_kernel(
    place, q_ref, own_ref, other_ref, wk_ref, wv_ref, out_ref, key_buf, turn_buf, value_buf, *, slots, scales
):
    rows = q_ref.shape[1]
    heads = q_ref.shape[0]
    half = own_ref.shape[0] // (key_buf.shape[0] // rows)
    latent = wk_ref.shape[0]
    block, core = place[0], place[1]

    def expand(j, carry):
        for ref, side in ((own_ref, core), (other_ref, 1 - core)):
            part = ref[pl.ds(pl.multiple_of(j * half, half), half), :]
            at = pl.ds(pl.multiple_of(j * rows + side * half, half), half)
            wide = part[:, :latent]
            key_buf[at, :] = jnp.dot(wide, wk_ref[...], preferred_element_type=jnp.float32).astype(
                jnp.bfloat16
            )
            value_buf[at, :] = jnp.dot(
                wide, wv_ref[...], preferred_element_type=jnp.float32
            ).astype(jnp.bfloat16)
            turn_buf[at, :] = part[:, latent:]
        return carry

    lax.fori_loop(0, block + 1, expand, 0)

    def absorb(state, query, start, length, masked):
        at = pl.ds(pl.multiple_of(start, TILE), length)
        turned = turn_buf[at, :]
        out = []
        for h in range(heads):
            maximum, total, summed = state[h]
            keys = jnp.concatenate([key_buf[at, h * LANES : (h + 1) * LANES], turned], axis=1)
            scores = lax.dot_general(
                query[h], keys, (((1,), (1,)), ((), ())), preferred_element_type=jnp.float32
            )
            if masked:
                row = lax.broadcasted_iota(jnp.int32, scores.shape, 0)
                column = lax.broadcasted_iota(jnp.int32, scores.shape, 1)
                scores = jnp.where(column <= row, scores, FLOOR)
            new_max = jnp.maximum(maximum, jnp.max(scores, axis=1, keepdims=True))
            weights = jnp.exp2((scores - new_max) * scales[h])
            factor = jnp.exp2((maximum - new_max) * scales[h])
            total = total * factor
            for g in range(length // LANES):
                total = total + weights[:, g * LANES : (g + 1) * LANES]
            summed = summed * factor + jnp.dot(
                weights.astype(jnp.bfloat16),
                value_buf[at, h * LANES : (h + 1) * LANES],
                preferred_element_type=jnp.float32,
            )
            out.append((new_max, total, summed))
        return tuple(out)

    def tile(i, carry):
        at = pl.ds(pl.multiple_of(i * TILE, TILE), TILE)
        query = [q_ref[h, at, :] for h in range(heads)]
        state = tuple(
            (
                jnp.full((TILE, 1), FLOOR, jnp.float32),
                jnp.zeros((TILE, LANES), jnp.float32),
                jnp.zeros((TILE, LANES), jnp.float32),
            )
            for _ in range(heads)
        )
        state = lax.fori_loop(
            0, block, lambda j, s: absorb(s, query, j * rows, rows, False), state
        )
        base = block * rows
        state = lax.fori_loop(
            0, i, lambda j, s: absorb(s, query, base + j * TILE, TILE, False), state
        )
        state = absorb(state, query, base + i * TILE, TILE, True)
        columns = {}
        for h in range(heads):
            _, total, summed = state[h]
            value = summed / jnp.sum(total, axis=1, keepdims=True)
            columns[slots[h]] = columns[slots[h]] + value if slots[h] in columns else value
        for slot, value in columns.items():
            out_ref[at, slot * LANES : (slot + 1) * LANES] = value.astype(jnp.bfloat16)
        return carry

    lax.fori_loop(0, rows // TILE, tile, 0)


def on_device(
    resid,
    query_small,
    query_large,
    kv_latent,
    rope_key,
    kv_gain,
    up_key_small,
    up_value_small,
    up_key_large,
    up_value_large,
    out_weight,
    mix_gain,
    gate_weight,
    up_weight,
    down_weight,
    *,
    sp_count,
    tp_count,
):
    zs, ys = grid_of(sp_count)
    xs, cores = tp_count // 2, 2
    rows = kv_latent.shape[0]
    half = rows // cores
    sp_index = lax.axis_index("sp").astype(jnp.int32)
    core = (lax.axis_index("tp") % cores).astype(jnp.int32)
    positions = sp_index * rows + jnp.arange(rows, dtype=jnp.int32)
    angle_cos, angle_sin = angles(positions, ROTARY)
    packed = jnp.concatenate(
        [
            norm_rows(kv_latent, kv_gain),
            padded(rotate(rope_key, angle_cos, angle_sin), 0, LANES),
        ],
        axis=1,
    )
    packed = lax.dynamic_slice_in_dim(packed, core * half, half, 0)
    own_half = gather_rows(packed, "sp", zs, ys)
    other_half = shift(own_half, "tp", xs, cores, 0, 1)

    gate_whole = lax.all_gather(gate_weight, "sp", axis=0, tiled=True)
    up_whole = lax.all_gather(up_weight, "sp", axis=0, tiled=True)
    down_whole = gather_rows(down_weight, "sp", zs, ys)

    heads_small = up_key_small.shape[1] // NOPE_SMALL
    heads_large = up_key_large.shape[1] // NOPE_LARGE
    heads = heads_small + heads_large

    def queries(query, count, nope):
        shaped = query.reshape(rows, count, -1)
        turned = rotate(shaped[..., nope:], angle_cos[:, None, :], angle_sin[:, None, :])
        both = jnp.concatenate(
            [padded(shaped[..., :nope], 0, LANES), padded(turned, 0, LANES)], axis=-1
        )
        return jnp.transpose(both, (1, 0, 2))

    query = jnp.concatenate(
        [
            queries(query_small, heads_small, NOPE_SMALL),
            queries(query_large, heads_large, NOPE_LARGE),
        ],
        axis=0,
    )
    key_columns, value_columns, slots, scales = [], [], [], []
    for h in range(heads_small):
        key_columns.append(
            padded(up_key_small[:, h * NOPE_SMALL : (h + 1) * NOPE_SMALL], 0, LANES)
        )
        value_columns.append(
            padded(
                up_value_small[:, h * VALUE_SMALL : (h + 1) * VALUE_SMALL],
                h % 2 * VALUE_SMALL,
                LANES,
            )
        )
        slots.append(h // 2)
        scales.append(LOG2E / math.sqrt(NOPE_SMALL + ROTARY))
    for h in range(heads_large):
        slots.append((heads_small + 1) // 2 + h)
        scales.append(LOG2E / math.sqrt(NOPE_LARGE + ROTARY))
    wk = jnp.concatenate(key_columns + [up_key_large], axis=1)
    wv = jnp.concatenate(value_columns + [up_value_large], axis=1)
    width = (max(slots) + 1) * LANES
    length = rows * sp_count
    vmem = pl.BlockSpec(memory_space=pltpu.VMEM)
    attended = pl.pallas_call(
        lambda *refs: attend_kernel(*refs, slots=slots, scales=scales),
        out_shape=jax.ShapeDtypeStruct((rows, width), jnp.bfloat16),
        in_specs=[pl.BlockSpec(memory_space=pltpu.SMEM)] + [vmem] * 5,
        out_specs=vmem,
        scratch_shapes=[
            pltpu.VMEM((length, heads * LANES), jnp.bfloat16),
            pltpu.VMEM((length, LANES), jnp.bfloat16),
            pltpu.VMEM((length, heads * LANES), jnp.bfloat16),
        ],
        compiler_params=pltpu.CompilerParams(vmem_limit_bytes=44 * 1024 * 1024),
        name="attend",
    )(jnp.stack([sp_index, core]), query, own_half, other_half, wk, wv)
    small_width = heads_small * VALUE_SMALL
    large_width = heads_large * VALUE_LARGE
    if heads_small % 2:
        attended = jnp.concatenate(
            [attended[:, :small_width], attended[:, width - large_width :]], axis=1
        )
    mine = rows // tp_count
    border = HEADS_SMALL * VALUE_SMALL
    shared = lax.all_to_all(
        attended.reshape(tp_count, mine, small_width + large_width), "tp", 0, 0
    )
    all_small = jnp.transpose(shared[..., :small_width], (1, 0, 2)).reshape(mine, -1)
    all_large = jnp.transpose(shared[..., small_width:], (1, 0, 2)).reshape(mine, -1)
    mixed = jnp.dot(all_small, out_weight[:border], preferred_element_type=jnp.float32)
    mixed = mixed + jnp.dot(all_large, out_weight[border:], preferred_element_type=jnp.float32)
    middle = (resid.astype(jnp.float32) + mixed).astype(jnp.bfloat16)
    mixer_in = norm_rows(middle, mix_gain)

    far = [mixer_in] + [shift(mixer_in, "tp", xs, cores, a, 0) for a in range(1, xs)]
    pairs = [jnp.concatenate([f, shift(f, "tp", xs, cores, 0, 1)], axis=0) for f in far]
    hidden = []
    for piece in pairs:
        gate = jnp.dot(piece, gate_whole, preferred_element_type=jnp.float32)
        upward = jnp.dot(piece, up_whole, preferred_element_type=jnp.float32)
        hidden.append((jax.nn.silu(gate) * upward).astype(jnp.bfloat16))
    arrived = []
    for a in reversed(range(xs)):
        part = lax.dot_general(
            hidden[a], down_whole, (((1,), (1,)), ((), ())), preferred_element_type=jnp.float32
        ).astype(jnp.bfloat16)
        beside = shift(part[mine:], "tp", xs, cores, 0, 1)
        both = part[:mine].astype(jnp.float32) + beside.astype(jnp.float32)
        if a:
            both = shift(both.astype(jnp.bfloat16), "tp", xs, cores, -a, 0).astype(jnp.float32)
        arrived.append(both)
    total = middle.astype(jnp.float32)
    for part in arrived[::-1]:
        total = total + part
    return total.astype(jnp.bfloat16)


def solution(mesh):
    placed = (
        P(("sp", "tp"), None),
        P("sp", "tp"),
        P("sp", "tp"),
        P("sp", None),
        P("sp", None),
        P(),
        P(None, "tp"),
        P(None, "tp"),
        P(None, "tp"),
        P(None, "tp"),
        P(),
        P(),
        P("sp", "tp"),
        P("sp", "tp"),
        P("sp", "tp"),
    )
    sizes = {"sp_count": mesh.shape["sp"], "tp_count": mesh.shape["tp"]}
    return jax.shard_map(
        lambda *arrays: on_device(*arrays, **sizes), mesh=mesh, in_specs=placed, out_specs=P(("sp", "tp"), None), check_vma=False
    )
```
